32 devices in a mesh: sp: 8 (over z, y), tp: 4 (over x, core).
Axes of the slice: x: 2, y: 2, z: 4, core: 2. Of those that a mesh axis runs over, the one named last changes fastest.
Arguments:
- resid: bfloat16 [2048, 2048], P(('sp', 'tp')), may hold values from -6 to 6
- query_a: bfloat16 [2048, 4, 128], P('sp', 'tp')
- key_a: bfloat16 [2048, 4, 128], P('sp', 'tp')
- value_a: bfloat16 [2048, 4, 128], P('sp', 'tp'), may hold values from -6 to 6
- query_b: bfloat16 [2048, 4, 256], P('sp', 'tp')
- key_b: bfloat16 [2048, 4, 256], P('sp', 'tp')
- value_b: bfloat16 [2048, 4, 128], P('sp', 'tp'), may hold values from -6 to 6
- lambda_a: float32 [4], P('tp'), may hold values from 0.3 to 0.8
- lambda_b: float32 [4], P('tp'), may hold values from 0.3 to 0.8
- head_gain: float32 [128], replicated, may hold values from 0.1 to 1.9
- out_weight: bfloat16 [1024, 2048], replicated, may hold values from -0.1875 to 0.1875
- norm_gain: float32 [2048], replicated, may hold values from 0.1 to 1.9
- expert_ids: int32 [2048, 4], P(('sp', 'tp')), may hold values from 0 to 31, all different within a row; in each aligned block of 64 rows (0 to 63, 64 to 127, ...) at most 16 rows name the same one
- expert_mix: float32 [2048, 4], P(('sp', 'tp')), may hold values from 0.2 to 1
- gate_experts: bfloat16 [32, 2048, 1024], P(('sp', 'tp')), may hold values from -0.125 to 0.125
- up_experts: bfloat16 [32, 2048, 1024], P(('sp', 'tp')), may hold values from -0.125 to 0.125
- down_experts: bfloat16 [32, 1024, 2048], P(('sp', 'tp')), may hold values from -0.1875 to 0.1875
- shared_gate: bfloat16 [2048, 512], replicated, may hold values from -0.125 to 0.125
- shared_up: bfloat16 [2048, 512], replicated, may hold values from -0.125 to 0.125
- shared_down: bfloat16 [512, 2048], replicated, may hold values from -0.25 to 0.25
Outputs:
- layer_out: bfloat16 [2048, 2048], P(('sp', 'tp'))
The draws below stay inside these ranges and needn't reach their ends.
Inputs may be any that keep to these rules, and one draw needn't show every extreme that they name: `expert_ids`: in each aligned block of 64 rows (the rows of one device) no expert is named more than 16 times, a bound that some block reaches.
All inputs are finite; a program needn't handle non-finite values.
Results may differ from the reference program's by a relative error of at most 0.017.
Values may be sent and summed in bfloat16 or wider, within the bound.
No kernel may reach another device: no remote copies, remote signals or barrier semaphores. Data moves between devices by JAX's collectives and lax.ppermute only.
A program may use at most 128 MiB of HBM per device.

```python
import math
import jax
import jax.numpy as jnp
import numpy as np
from jax import lax

D = 2048
HA = 4
HB = 4
DA = 64
DB = 128
DV = 128
EFF = 1024
SFF = 512
TOPK = 4
TOK_DEV = 64
TOKENS = 2048
EXPERTS = 32
CAP = 16
N_SP = 8
N_TP = 4


def drawn_pair(key, tag, head_count, width):
    base = jax.random.fold_in(key, tag)
    query_key, key_key = jax.random.split(base)
    queries = 1.3 * jax.random.normal(query_key, (TOKENS, head_count, width), jnp.float32)
    keys = 1.3 * jax.random.normal(key_key, (TOKENS, head_count, width), jnp.float32)
    return (queries.astype(jnp.bfloat16), keys.astype(jnp.bfloat16))


def draw_query_a(key, part):
    return drawn_pair(key, 11, HA, 2 * DA)[0]


def draw_key_a(key, part):
    return drawn_pair(key, 11, HA, 2 * DA)[1]


def draw_query_b(key, part):
    return drawn_pair(key, 23, HB, 2 * DB)[0]


def draw_key_b(key, part):
    return drawn_pair(key, 23, HB, 2 * DB)[1]


def steps_of(rng, extent, pieces, smallest, high):
    def one(axis_at, parts):
        heights = jax.random.uniform(jax.random.fold_in(jax.random.fold_in(rng, 6), axis_at), (parts,), jnp.float32, smallest / len(pieces), high / len(pieces))
        return jnp.repeat(jnp.exp(heights), extent[axis_at] // parts).reshape((-1,) + (1,) * (len(extent) - axis_at - 1))

    gain = one(*pieces[0])
    for cut in pieces[1:]:
        gain = gain * one(*cut)
    return gain


def shared_out(own_key, own, number, rows, amount, top, reach, slope):
    order = jax.random.permutation(own_key, amount)
    packed, usual = load_shares(amount, rows * top, reach, slope, True), load_shares(amount, rows * top, reach, slope, False)
    places = jnp.arange(amount)

    def named(sizes, turn):
        used = int((sizes > 0).sum())
        fixed = max(1, used // 4)
        passed = fixed + (places - fixed + turn * (used - fixed)) % max(1, amount - fixed)
        return jnp.zeros((amount,), jnp.int32).at[order[jnp.where(places < fixed, places, passed)]].set(jnp.asarray(sizes, jnp.int32))

    sizes = jnp.where(number % 4 == 0, named(packed, number // 4), named(usual, number - number // 4 - 1))
    mixed = jax.random.permutation(jax.random.fold_in(own, 3), amount)
    giver, sink = mixed[0:amount // 2 * 2:2], mixed[1:amount // 2 * 2:2]
    slack = jnp.minimum(sizes[giver] - 1, reach - sizes[sink]) // 2
    slack = jnp.where((giver == order[0]) | (sink == order[0]) | (sizes[sink] == 0), 0, jnp.maximum(slack, 0))
    passed = jax.random.randint(jax.random.fold_in(own, 4), (amount // 2,), 0, 1 << 20) % (slack + 1)
    sizes = sizes.at[giver].add(-passed).at[sink].add(passed)
    items = jnp.searchsorted(jnp.cumsum(sizes), jnp.arange(rows * top), side="right").astype(jnp.int32)
    grid = items.reshape(top, rows).T
    grid = grid[jax.random.permutation(jax.random.fold_in(own, 1), rows)]
    turn = jax.random.randint(jax.random.fold_in(own, 2), (rows, 1), 0, top)
    return jnp.take_along_axis(grid, (jnp.arange(top)[None, :] + turn) % top, axis=1)


def load_shares(number_of, total, limit, skew, full):
    portions = [(1 << 20) // math.isqrt(grade ** skew) + 1 for grade in range(1, number_of + 1)]
    largest = limit if full else min(limit, max(-(-total // number_of), total * portions[0] // sum(portions)))
    least = 1 if total - largest >= number_of - 1 else 0
    counts, rest = [largest] + [least] * (number_of - 1), total - largest - least * (number_of - 1)
    while rest > 0:
        free = [i for i in range(1, number_of) if counts[i] < largest] or [i for i in range(1, number_of) if counts[i] < limit]
        whole, remaining = sum([portions[i] for i in free]), rest
        for i in free:
            addition = min(limit - counts[i], max(1, remaining * portions[i] // whole), rest)
            counts[i] = counts[i] + addition
            rest = rest - addition
    return np.array(counts)


def noise(stream_key, extent, scale, reach, pieces=(), kind=jnp.bfloat16):
    values = jax.random.normal(stream_key, extent, jnp.float32) * scale
    if len(pieces) > 0:
        values = steps_of(stream_key, extent, pieces, -0.22, 0.18) * values
    return jnp.clip(values, min=-reach, max=reach).astype(kind)


def setup_inputs(seed: int = 0) -> dict:
    seeds = jax.random.split(jax.random.key(seed), 21)
    resid = noise(seeds[0], (TOKENS, D), 1.0, 6.0, ((0, 32),))
    query_a = draw_query_a(jax.random.fold_in(seeds[20], 71), 0)
    key_a = draw_key_a(jax.random.fold_in(seeds[20], 71), 0)
    value_a = noise(seeds[3], (TOKENS, HA, DV), 1.0, 6.0, ((0, 8), (1, 4)))
    query_b = draw_query_b(jax.random.fold_in(seeds[20], 71), 0)
    key_b = draw_key_b(jax.random.fold_in(seeds[20], 71), 0)
    value_b = noise(seeds[6], (TOKENS, HB, DV), 1.0, 6.0, ((0, 8), (1, 4)))
    lambda_a = jnp.clip(0.3 + 0.5 * jax.random.uniform(seeds[7], (HA,), jnp.float32) ** steps_of(seeds[7], (HA,), ((0, 4),), -0.2, 0.2), 0.3, 0.8)
    lambda_b = jnp.clip(0.3 + 0.5 * jax.random.uniform(seeds[8], (HB,), jnp.float32) ** steps_of(seeds[8], (HB,), ((0, 4),), -0.2, 0.2), 0.3, 0.8)
    head_gain = jnp.clip(1.0 + 0.18 * jax.random.normal(seeds[9], (DV,), jnp.float32), 0.1, 1.9)
    out_weight = noise(seeds[10], ((HA + HB) * DV, D), ((HA + HB) * DV) ** -0.5, 0.1875)
    norm_gain = jnp.clip(1.0 + 0.18 * jax.random.normal(seeds[11], (D,), jnp.float32), 0.1, 1.9)
    expert_ids_keys = jax.random.split(jax.random.fold_in(seeds[12], 1), TOKENS // TOK_DEV)
    expert_ids_turns = jax.random.permutation(jax.random.fold_in(seeds[12], 3), TOKENS // TOK_DEV)
    expert_ids = jax.vmap(lambda own, number: shared_out(jax.random.fold_in(seeds[12], 2), own, number, TOK_DEV, EXPERTS, TOPK, CAP, 2))(expert_ids_keys, expert_ids_turns).reshape((TOKENS, TOPK))
    expert_mix = jnp.clip(jnp.exp(math.log(1.0) - 1.609438 * jax.random.uniform(seeds[13], (TOKENS, TOPK), jnp.float32) ** steps_of(seeds[13], (TOKENS, TOPK), ((0, 32),), -0.2, 0.2)), 0.2, 1.0)
    gate_experts = noise(seeds[14], (EXPERTS, D, EFF), D ** -0.5, 0.125, ((0, 32),))
    up_experts = noise(seeds[15], (EXPERTS, D, EFF), D ** -0.5, 0.125, ((0, 32),))
    down_experts = noise(seeds[16], (EXPERTS, EFF, D), EFF ** -0.5, 0.1875, ((0, 32),))
    shared_gate = noise(seeds[17], (D, SFF), D ** -0.5, 0.125)
    shared_up = noise(seeds[18], (D, SFF), D ** -0.5, 0.125)
    shared_down = noise(seeds[19], (SFF, D), SFF ** -0.5, 0.25)
    return dict(resid=resid, query_a=query_a, key_a=key_a, value_a=value_a, query_b=query_b, key_b=key_b, value_b=value_b, lambda_a=lambda_a, lambda_b=lambda_b, head_gain=head_gain, out_weight=out_weight, norm_gain=norm_gain, expert_ids=expert_ids, expert_mix=expert_mix, gate_experts=gate_experts, up_experts=up_experts, down_experts=down_experts, shared_gate=shared_gate, shared_up=shared_up, shared_down=shared_down)


NEG_FILL = -1e+30
EPSILON = 1e-05
HEAD_SCALE = 0.8

def group_attention(queries, keys, values, lambdas, head_gain):
    seq_total = queries.shape[0]
    map_width = queries.shape[2] // 2
    head_count = queries.shape[1]
    value_width = values.shape[2]
    block_rows = min(512, seq_total)
    key_float = keys.astype(jnp.float32)
    value_float = values.astype(jnp.float32)
    key_pos = jnp.arange(seq_total, dtype=jnp.int32)
    scaling = map_width ** (-0.5)

    def one_block(begin_row):
        query_block = lax.dynamic_slice_in_dim(queries, begin_row, block_rows, 0).astype(jnp.float32)
        query_pos = begin_row + jnp.arange(block_rows, dtype=jnp.int32)
        causal = (key_pos[None, :] <= query_pos[:, None])[None]
        results = []
        for map_index in range(2):
            low_col = map_index * map_width
            scores = jnp.einsum('qhd,khd->hqk', query_block[:, :, low_col:low_col + map_width], key_float[:, :, low_col:low_col + map_width]) * scaling
            scores = jnp.where(causal, scores, NEG_FILL)
            row_top = lax.optimization_barrier(jnp.max(scores, axis=2, keepdims=True))
            exponent = jnp.where(causal, jnp.exp(scores - row_top), 0.0)
            denoms = lax.optimization_barrier(jnp.sum(exponent, axis=2))
            rounded = lax.optimization_barrier(exponent.astype(jnp.bfloat16)).astype(jnp.float32)
            numerator = jnp.einsum('hqk,khe->qhe', rounded, value_float)
            results.append(numerator / jnp.transpose(denoms)[:, :, None])
        differ = results[0] - lambdas[None, :, None] * results[1]
        scale_rms = lax.rsqrt(lax.optimization_barrier(jnp.mean(differ * differ, axis=2, keepdims=True)) + EPSILON)
        return (differ * scale_rms * head_gain[None, None, :] * HEAD_SCALE).astype(jnp.bfloat16)
    starts = jnp.arange(seq_total // block_rows, dtype=jnp.int32) * block_rows
    outputs = lax.map(one_block, starts)
    return outputs.reshape(seq_total, head_count, value_width)

def swiglu_rows(row_set, w_gate, w_up, w_down):
    gate_val = jnp.dot(row_set, w_gate, preferred_element_type=jnp.float32)
    up_val = jnp.dot(row_set, w_up, preferred_element_type=jnp.float32)
    hidden = (jax.nn.silu(gate_val) * up_val).astype(jnp.bfloat16)
    return jnp.dot(hidden, w_down, preferred_element_type=jnp.float32)

def reference(resid, query_a, key_a, value_a, query_b, key_b, value_b, lambda_a, lambda_b, head_gain, out_weight, norm_gain, expert_ids, expert_mix, gate_experts, up_experts, down_experts, shared_gate, shared_up, shared_down):
    seq_total = resid.shape[0]
    heads_a = group_attention(query_a, key_a, value_a, lambda_a, head_gain)
    heads_b = group_attention(query_b, key_b, value_b, lambda_b, head_gain)
    joined = jnp.concatenate([heads_a.reshape(seq_total, -1), heads_b.reshape(seq_total, -1)], axis=1)
    project = jnp.dot(joined, out_weight, preferred_element_type=jnp.float32)
    middle = (resid.astype(jnp.float32) + project).astype(jnp.bfloat16)
    middle_f = middle.astype(jnp.float32)
    normed = (middle_f * lax.rsqrt(lax.optimization_barrier(jnp.mean(middle_f * middle_f, axis=1, keepdims=True)) + EPSILON) * norm_gain[None, :]).astype(jnp.bfloat16)
    shared = swiglu_rows(normed, shared_gate, shared_up, shared_down)
    top_count = expert_ids.shape[1]
    flat_ids = expert_ids.reshape(-1).astype(jnp.int32)
    flat_mix = expert_mix.reshape(-1)
    expert_count = gate_experts.shape[0]
    sorted_pairs = jnp.argsort(flat_ids, stable=True).astype(jnp.int32)
    load_counts = lax.optimization_barrier(jnp.sum((flat_ids[:, None] == jnp.arange(expert_count, dtype=jnp.int32)[None, :]).astype(jnp.int32), axis=0))
    offsets = (jnp.cumsum(load_counts) - load_counts).astype(jnp.int32)
    most_rows = N_SP * N_TP * CAP
    padded_pairs = jnp.concatenate([sorted_pairs, jnp.zeros((most_rows,), jnp.int32)])

    def one_expert(routed, inputs):
        expert_index, w_gate, w_up, w_down = inputs
        picked = lax.dynamic_slice_in_dim(padded_pairs, offsets[expert_index], most_rows, 0)
        is_valid = jnp.arange(most_rows, dtype=jnp.int32) < load_counts[expert_index]
        token_rows = (picked // top_count).astype(jnp.int32)
        result = swiglu_rows(normed[token_rows], w_gate, w_up, w_down)
        result = lax.optimization_barrier(result.astype(jnp.bfloat16)).astype(jnp.float32)
        weights = jnp.where(is_valid, flat_mix[picked], 0.0)
        return (routed.at[token_rows].add(result * weights[:, None]), None)
    routed = lax.scan(one_expert, jnp.zeros((seq_total, D), jnp.float32), (jnp.arange(expert_count, dtype=jnp.int32), gate_experts, up_experts, down_experts))[0]
    return (middle_f + shared + routed).astype(jnp.bfloat16)
```

```python
import jax
import jax.numpy as jnp
from jax import lax
from jax.experimental import pallas as pl
from jax.experimental.pallas import tpu as pltpu
from jax.sharding import PartitionSpec as P

NEG_FILL = -1e30
EPSILON = 1e-05
HEAD_SCALE = 0.8
MAPS = 4


def attend_kernel(
    factor_ref, query_ref, key_ref, value_ref, out_ref, *, chunk, rows, block, tok_dev, part
):
    split = factor_ref[0, 0].astype(jnp.int32)
    scaling = factor_ref[0, 1]
    factor = factor_ref[0, 2]
    total = query_ref.shape[0]
    for begin in range(0, total, chunk):
        sources = chunk // rows
        first = begin // rows
        span = (first + sources) * block
        query = query_ref[begin : begin + chunk, :]
        scores = (
            lax.dot_general(
                query,
                key_ref[:span, :],
                (((1,), (1,)), ((), ())),
                preferred_element_type=jnp.float32,
            )
            * scaling
        )
        row = lax.broadcasted_iota(jnp.int32, (chunk, 1), 0)
        inner = row % rows
        pos = (first + row // rows) * block + (inner // part) * tok_dev + split * part + inner % part
        key_pos = lax.broadcasted_iota(jnp.int32, (chunk, span), 1)
        causal = key_pos <= pos
        scores = jnp.where(causal, scores, NEG_FILL)
        top = jnp.max(scores, axis=1, keepdims=True)
        exponent = jnp.exp(scores - top)
        denom = jnp.sum(exponent, axis=1, keepdims=True)
        numer = jnp.dot(
            exponent.astype(jnp.bfloat16), value_ref[:span, :], preferred_element_type=jnp.float32
        )
        out_ref[begin : begin + chunk, :] = (numer * (factor / denom)).astype(jnp.bfloat16)


def swiglu_rows(row_set, w_gate, w_up, w_down):
    gate_val = jnp.dot(row_set, w_gate, preferred_element_type=jnp.float32)
    up_val = jnp.dot(row_set, w_up, preferred_element_type=jnp.float32)
    hidden = (jax.nn.silu(gate_val) * up_val).astype(jnp.bfloat16)
    return jnp.dot(hidden, w_down, preferred_element_type=jnp.float32)


def widen(array, width):
    return jnp.pad(array, ((0, 0), (0, width - array.shape[1])))


def attention(
    query_a, key_a, value_a, query_b, key_b, value_b, lambda_a, lambda_b, head_gain, tok_dev
):
    sp_count = lax.axis_size("sp")
    tp_count = lax.axis_size("tp")
    splits = sp_count // MAPS
    block = query_a.shape[0]
    width_a, width_b = query_a.shape[2] // 2, query_b.shape[2] // 2
    width = max(width_a, width_b)
    value_width = value_a.shape[2]
    part = tok_dev // splits
    rows = block // splits

    def by_map(array_a, array_b):
        array_a, array_b = array_a[:, 0], array_b[:, 0]
        return [
            widen(array_a[:, :width_a], width),
            widen(array_a[:, width_a:], width),
            array_b[:, :width_b],
            array_b[:, width_b:],
        ]

    keys = by_map(key_a, key_b)
    queries = by_map(query_a, query_b)
    values = [value_a[:, 0]] * 2 + [value_b[:, 0]] * 2
    pieces = []
    for unit in range(MAPS):
        shares = queries[unit].reshape(tp_count, splits, part, width)
        for split in range(splits):
            pieces.append(
                jnp.concatenate(
                    [keys[unit], values[unit], shares[:, split].reshape(rows, width)], axis=0
                )
            )
    packed = jnp.stack(pieces)
    got = lax.all_to_all(packed, "sp", split_axis=0, concat_axis=0, tiled=True)
    key_all = got[:, :block].reshape(-1, width)
    value_all = got[:, block : 2 * block].reshape(-1, value_width)
    query_all = got[:, 2 * block :].reshape(-1, width)
    place = lax.axis_index("sp")
    unit, split = place // splits, place % splits
    in_a = unit < 2
    scaling = jnp.where(in_a, width_a ** (-0.5), width_b ** (-0.5))
    lam = jnp.where(in_a, lambda_a[0], lambda_b[0])
    factor = jnp.where(unit % 2 == 1, lam, 1.0)
    scalars = jnp.stack([split.astype(jnp.float32), scaling, factor])[None]
    total = query_all.shape[0]
    chunk = rows * max(1, min(sp_count, 256 // rows))
    outs = pl.pallas_call(
        lambda *refs: attend_kernel(
            *refs, chunk=chunk, rows=rows, block=block, tok_dev=tok_dev, part=part
        ),
        out_shape=jax.ShapeDtypeStruct((total, value_width), jnp.bfloat16),
        in_specs=[pl.BlockSpec(memory_space=pltpu.SMEM)]
        + [pl.BlockSpec(memory_space=pltpu.VMEM)] * 3,
        out_specs=pl.BlockSpec(memory_space=pltpu.VMEM),
        name="attend",
    )(scalars, query_all, key_all, value_all)
    back = lax.all_to_all(
        outs.reshape(sp_count * tp_count, part, value_width),
        ("sp", "tp"),
        split_axis=0,
        concat_axis=0,
        tiled=True,
    )
    back = back.reshape(2, 2, splits, tp_count, part, value_width).astype(jnp.float32)
    differ = back[:, 0] - back[:, 1]
    scale_rms = lax.rsqrt(jnp.mean(differ * differ, axis=-1, keepdims=True) + EPSILON)
    heads = (differ * scale_rms * head_gain * HEAD_SCALE).astype(jnp.bfloat16)
    return jnp.transpose(heads, (1, 3, 0, 2, 4)).reshape(tok_dev, -1)


def per_device(
    resid,
    query_a,
    key_a,
    value_a,
    query_b,
    key_b,
    value_b,
    lambda_a,
    lambda_b,
    head_gain,
    out_weight,
    norm_gain,
    expert_ids,
    expert_mix,
    gate_experts,
    up_experts,
    down_experts,
    shared_gate,
    shared_up,
    shared_down,
):
    tok_dev = resid.shape[0]
    joined = attention(
        query_a, key_a, value_a, query_b, key_b, value_b, lambda_a, lambda_b, head_gain, tok_dev
    )
    project = jnp.dot(joined, out_weight, preferred_element_type=jnp.float32)
    middle = (resid.astype(jnp.float32) + project).astype(jnp.bfloat16)
    middle_f = middle.astype(jnp.float32)
    normed = (
        middle_f
        * lax.rsqrt(jnp.mean(middle_f * middle_f, axis=1, keepdims=True) + EPSILON)
        * norm_gain[None, :]
    ).astype(jnp.bfloat16)
    shared = swiglu_rows(normed, shared_gate, shared_up, shared_down)
    top_count = expert_ids.shape[1]
    model_width = normed.shape[1]
    sp_count = lax.axis_size("sp")
    tp_count = lax.axis_size("tp")
    expert_total = sp_count * tp_count
    pair_count = tok_dev * top_count
    capacity = max(2, 2 * pair_count // expert_total)
    hits = expert_ids[:, :, None] == jnp.arange(expert_total, dtype=jnp.int32)
    named = jnp.any(hits, axis=1).astype(jnp.float32)
    mixes = jnp.sum(jnp.where(hits, expert_mix[:, :, None], 0.0), axis=1)
    earlier = jnp.tril(jnp.ones((tok_dev, tok_dev), jnp.float32), -1)
    rank = jnp.dot(earlier, named)
    slots = jnp.arange(capacity, dtype=jnp.float32)
    picks = (rank.T[:, None, :] == slots[None, :, None]) & (named.T[:, None, :] > 0)
    pick_rows = picks.astype(jnp.bfloat16).reshape(expert_total * capacity, tok_dev)
    send_rows = (
        jnp.dot(pick_rows, normed, preferred_element_type=jnp.float32)
        .astype(jnp.bfloat16)
        .reshape(expert_total, capacity, model_width)
    )
    arrived = lax.all_to_all(send_rows, ("sp", "tp"), split_axis=0, concat_axis=0, tiled=True)
    arrived_shape = arrived.shape
    flat_rows = arrived.reshape(-1, arrived_shape[-1])
    result = swiglu_rows(flat_rows, gate_experts[0], up_experts[0], down_experts[0]).astype(
        jnp.bfloat16
    )
    finished = result.reshape(arrived_shape)
    returned = lax.all_to_all(finished, ("sp", "tp"), split_axis=0, concat_axis=0, tiled=True)
    mix_picks = jnp.where(
        (rank[:, :, None] == slots) & (named[:, :, None] > 0), mixes[:, :, None], 0.0
    ).reshape(tok_dev, -1)
    mix_high = mix_picks.astype(jnp.bfloat16)
    mix_low = (mix_picks - mix_high.astype(jnp.float32)).astype(jnp.bfloat16)
    both = jnp.dot(
        jnp.concatenate([mix_high, mix_low], axis=0),
        returned.reshape(-1, model_width),
        preferred_element_type=jnp.float32,
    )
    routed = both[:tok_dev] + both[tok_dev:]
    return (middle_f + shared + routed).astype(jnp.bfloat16)


def solution(mesh):
    in_specs = (
        P(("sp", "tp"), None),
        P("sp", "tp", None),
        P("sp", "tp", None),
        P("sp", "tp", None),
        P("sp", "tp", None),
        P("sp", "tp", None),
        P("sp", "tp", None),
        P("tp"),
        P("tp"),
        P(),
        P(),
        P(),
        P(("sp", "tp"), None),
        P(("sp", "tp"), None),
        P(("sp", "tp"), None, None),
        P(("sp", "tp"), None, None),
        P(("sp", "tp"), None, None),
        P(),
        P(),
        P(),
    )
    out_specs = P(("sp", "tp"), None)
    return jax.shard_map(
        per_device, mesh=mesh, in_specs=in_specs, out_specs=out_specs, check_vma=False
    )
```

```python
import jax
import jax.numpy as jnp
from jax import lax
from jax.experimental import pallas as pl
from jax.experimental.pallas import tpu as pltpu
from jax.sharding import PartitionSpec as P

NEG_FILL = -1e30
EPSILON = 1e-05
HEAD_SCALE = 0.8
MAPS = 4


def attend_kernel(
    factor_ref, got_ref, out_ref, *, chunk, rows, block, tok_dev, part
):
    split = factor_ref[0, 0].astype(jnp.int32)
    scaling = factor_ref[0, 1]
    factor = factor_ref[0, 2]
    width = got_ref.shape[2]
    sources = chunk // rows
    for first in range(0, got_ref.shape[0], sources):
        begin = first * rows
        last = first + sources
        span = last * block
        query = got_ref[first:last, 2 * block :, :].reshape(chunk, width)
        scores = (
            lax.dot_general(
                query,
                got_ref[:last, :block, :].reshape(span, width),
                (((1,), (1,)), ((), ())),
                preferred_element_type=jnp.float32,
            )
            * scaling
        )
        row = lax.broadcasted_iota(jnp.int32, (chunk, 1), 0)
        inner = row % rows
        pos = (first + row // rows) * block + (inner // part) * tok_dev + split * part + inner % part
        key_pos = lax.broadcasted_iota(jnp.int32, (chunk, span), 1)
        causal = key_pos <= pos
        scores = jnp.where(causal, scores, NEG_FILL)
        top = jnp.max(scores, axis=1, keepdims=True)
        exponent = jnp.exp(scores - top)
        denom = jnp.sum(exponent, axis=1, keepdims=True)
        numer = jnp.dot(
            exponent.astype(jnp.bfloat16),
            got_ref[:last, block : 2 * block, :].reshape(span, width),
            preferred_element_type=jnp.float32,
        )
        out_ref[begin : begin + chunk, :] = (numer * (factor / denom)).astype(jnp.bfloat16)


def swiglu_rows(row_set, w_gate, w_up, w_down):
    gate_val = jnp.dot(row_set, w_gate, preferred_element_type=jnp.float32)
    up_val = jnp.dot(row_set, w_up, preferred_element_type=jnp.float32)
    hidden = (jax.nn.silu(gate_val) * up_val).astype(jnp.bfloat16)
    return jnp.dot(hidden, w_down, preferred_element_type=jnp.float32)


def pack_kernel(qa_ref, ka_ref, va_ref, qb_ref, kb_ref, vb_ref, out_ref, *, splits, tok_dev):
    block = ka_ref.shape[0]
    width = out_ref.shape[2]
    part = tok_dev // splits
    half = width // 2
    lane = lax.broadcasted_iota(jnp.int32, (block, width), 1)
    query_a = qa_ref[...]
    zero = jnp.zeros_like(query_a)
    queries = [
        jnp.where(lane < half, query_a, zero),
        jnp.where(lane >= half, query_a, zero),
        qb_ref[:, :width],
        qb_ref[:, width:],
    ]
    keys = [ka_ref[...], ka_ref[...], kb_ref[:, :width], kb_ref[:, width:]]
    values = [va_ref[...], va_ref[...], vb_ref[...], vb_ref[...]]
    for unit in range(MAPS):
        for split in range(splits):
            piece = unit * splits + split
            out_ref[piece, :block, :] = keys[unit]
            out_ref[piece, block : 2 * block, :] = values[unit]
            shares = queries[unit].reshape(block // tok_dev, splits, part, width)[:, split]
            out_ref[piece, 2 * block :, :] = shares.reshape(block // splits, width)


def expert_kernel(row_ref, gate_ref, up_ref, down_ref, out_ref, sum_ref):
    rows = row_ref[...]
    gate_val = jnp.dot(rows, gate_ref[...], preferred_element_type=jnp.float32)
    up_val = jnp.dot(rows, up_ref[...], preferred_element_type=jnp.float32)
    hidden = (gate_val * jax.nn.sigmoid(gate_val) * up_val).astype(jnp.bfloat16)
    result = jnp.dot(hidden, down_ref[...], preferred_element_type=jnp.float32)
    last = pl.num_programs(0) - 1

    @pl.when(pl.program_id(0) == 0)
    def _():
        sum_ref[...] = result

    @pl.when((pl.program_id(0) > 0) & (pl.program_id(0) < last))
    def _():
        sum_ref[...] += result

    @pl.when(pl.program_id(0) == last)
    def _():
        out_ref[...] = (sum_ref[...] + result).astype(jnp.bfloat16)


def expert_call(rows, w_gate, w_up, w_down):
    count, model_width = rows.shape
    hidden_width = w_gate.shape[1]
    step = hidden_width // 4
    return pl.pallas_call(
        expert_kernel,
        grid=(4,),
        out_shape=jax.ShapeDtypeStruct(rows.shape, jnp.bfloat16),
        in_specs=[
            pl.BlockSpec((count, model_width), lambda i: (0, 0)),
            pl.BlockSpec((model_width, step), lambda i: (0, i)),
            pl.BlockSpec((model_width, step), lambda i: (0, i)),
            pl.BlockSpec((step, model_width), lambda i: (i, 0)),
        ],
        out_specs=pl.BlockSpec((count, model_width), lambda i: (0, 0)),
        scratch_shapes=[pltpu.VMEM((count, model_width), jnp.float32)],
        name="expert",
    )(rows, w_gate, w_up, w_down)


def combine_kernel(mix_ref, row_ref, base_ref, out_ref):
    tokens = base_ref.shape[0]
    both = jnp.dot(mix_ref[...], row_ref[...], preferred_element_type=jnp.float32)
    out_ref[...] = (base_ref[...] + (both[:tokens] + both[tokens:])).astype(jnp.bfloat16)


def local_call(kernel, shape, name, operands, scalars=0):
    specs = [pl.BlockSpec(memory_space=pltpu.SMEM)] * scalars
    specs += [pl.BlockSpec(memory_space=pltpu.VMEM)] * (len(operands) - scalars)
    return pl.pallas_call(
        kernel,
        out_shape=jax.ShapeDtypeStruct(shape, jnp.bfloat16),
        in_specs=specs,
        out_specs=pl.BlockSpec(memory_space=pltpu.VMEM),
        name=name,
    )(*operands)


def attention(
    query_a, key_a, value_a, query_b, key_b, value_b, lambda_a, lambda_b, head_gain, tok_dev
):
    sp_count = lax.axis_size("sp")
    tp_count = lax.axis_size("tp")
    splits = sp_count // MAPS
    block = query_a.shape[0]
    width_a, width_b = query_a.shape[2] // 2, query_b.shape[2] // 2
    width = max(width_a, width_b)
    value_width = value_a.shape[2]
    part = tok_dev // splits
    rows = block // splits

    flat = [
        array.reshape(block, array.shape[2])
        for array in (query_a, key_a, value_a, query_b, key_b, value_b)
    ]
    packed = local_call(
        lambda *refs: pack_kernel(*refs, splits=splits, tok_dev=tok_dev),
        (sp_count, 2 * block + rows, width),
        "pack",
        flat,
    )
    got = lax.all_to_all(packed, "sp", split_axis=0, concat_axis=0, tiled=True)
    place = lax.axis_index("sp")
    unit, split = place // splits, place % splits
    in_a = unit < 2
    scaling = jnp.where(in_a, width_a ** (-0.5), width_b ** (-0.5))
    lam = jnp.where(in_a, lambda_a[0], lambda_b[0])
    factor = jnp.where(unit % 2 == 1, lam, 1.0)
    scalars = jnp.stack([split.astype(jnp.float32), scaling, factor])[None]
    total = sp_count * rows
    chunk = rows * max(1, min(sp_count, 256 // rows))
    outs = local_call(
        lambda *refs: attend_kernel(
            *refs, chunk=chunk, rows=rows, block=block, tok_dev=tok_dev, part=part
        ),
        (total, value_width),
        "attend",
        [scalars, got],
        scalars=1,
    )
    back = lax.all_to_all(
        outs.reshape(sp_count * tp_count, part, value_width),
        ("sp", "tp"),
        split_axis=0,
        concat_axis=0,
        tiled=True,
    )
    back = back.reshape(2, 2, splits, tp_count, part, value_width).astype(jnp.float32)
    differ = back[:, 0] - back[:, 1]
    scale_rms = lax.rsqrt(jnp.mean(differ * differ, axis=-1, keepdims=True) + EPSILON)
    heads = (differ * scale_rms * head_gain * HEAD_SCALE).astype(jnp.bfloat16)
    return jnp.transpose(heads, (1, 3, 0, 2, 4)).reshape(tok_dev, -1)


def per_device(
    resid,
    query_a,
    key_a,
    value_a,
    query_b,
    key_b,
    value_b,
    lambda_a,
    lambda_b,
    head_gain,
    out_weight,
    norm_gain,
    expert_ids,
    expert_mix,
    gate_experts,
    up_experts,
    down_experts,
    shared_gate,
    shared_up,
    shared_down,
):
    tok_dev = resid.shape[0]
    joined = attention(
        query_a, key_a, value_a, query_b, key_b, value_b, lambda_a, lambda_b, head_gain, tok_dev
    )
    project = jnp.dot(joined, out_weight, preferred_element_type=jnp.float32)
    middle = (resid.astype(jnp.float32) + project).astype(jnp.bfloat16)
    middle_f = middle.astype(jnp.float32)
    normed = (
        middle_f
        * lax.rsqrt(jnp.mean(middle_f * middle_f, axis=1, keepdims=True) + EPSILON)
        * norm_gain[None, :]
    ).astype(jnp.bfloat16)
    shared = swiglu_rows(normed, shared_gate, shared_up, shared_down)
    top_count = expert_ids.shape[1]
    model_width = normed.shape[1]
    sp_count = lax.axis_size("sp")
    tp_count = lax.axis_size("tp")
    expert_total = sp_count * tp_count
    pair_count = tok_dev * top_count
    capacity = max(2, 2 * pair_count // expert_total)
    hits = expert_ids[:, :, None] == jnp.arange(expert_total, dtype=jnp.int32)
    named = jnp.any(hits, axis=1).astype(jnp.float32)
    mixes = jnp.sum(jnp.where(hits, expert_mix[:, :, None], 0.0), axis=1)
    earlier = jnp.tril(jnp.ones((tok_dev, tok_dev), jnp.float32), -1)
    rank = jnp.dot(earlier, named)
    slots = jnp.arange(capacity, dtype=jnp.float32)
    picks = (rank.T[:, None, :] == slots[None, :, None]) & (named.T[:, None, :] > 0)
    pick_rows = picks.astype(jnp.bfloat16).reshape(expert_total * capacity, tok_dev)
    send_rows = (
        jnp.dot(pick_rows, normed, preferred_element_type=jnp.float32)
        .astype(jnp.bfloat16)
        .reshape(expert_total, capacity, model_width)
    )
    arrived = lax.all_to_all(send_rows, ("sp", "tp"), split_axis=0, concat_axis=0, tiled=True)
    arrived_shape = arrived.shape
    flat_rows = arrived.reshape(-1, arrived_shape[-1])
    result = expert_call(flat_rows, gate_experts[0], up_experts[0], down_experts[0])
    finished = result.reshape(arrived_shape)
    returned = lax.all_to_all(finished, ("sp", "tp"), split_axis=0, concat_axis=0, tiled=True)
    mix_picks = jnp.where(
        (rank[:, :, None] == slots) & (named[:, :, None] > 0), mixes[:, :, None], 0.0
    ).reshape(tok_dev, -1)
    mix_high = mix_picks.astype(jnp.bfloat16)
    mix_low = (mix_picks - mix_high.astype(jnp.float32)).astype(jnp.bfloat16)
    mix_rows = jnp.concatenate([mix_high, mix_low], axis=0)
    return local_call(
        combine_kernel,
        (tok_dev, model_width),
        "combine",
        [mix_rows, returned.reshape(-1, model_width), middle_f + shared],
    )


def solution(mesh):
    in_specs = (
        P(("sp", "tp"), None),
        P("sp", "tp", None),
        P("sp", "tp", None),
        P("sp", "tp", None),
        P("sp", "tp", None),
        P("sp", "tp", None),
        P("sp", "tp", None),
        P("tp"),
        P("tp"),
        P(),
        P(),
        P(),
        P(("sp", "tp"), None),
        P(("sp", "tp"), None),
        P(("sp", "tp"), None, None),
        P(("sp", "tp"), None, None),
        P(("sp", "tp"), None, None),
        P(),
        P(),
        P(),
    )
    out_specs = P(("sp", "tp"), None)
    return jax.shard_map(
        per_device, mesh=mesh, in_specs=in_specs, out_specs=out_specs, check_vma=False
    )
```
